32 devices in a mesh: grp: 2 (over y), ra: 4 (over z), cb: 2 (over x), dp: 2 (over core).
Axes of the slice: x: 2, y: 2, z: 4, core: 2. Of those that a mesh axis runs over, the one named last changes fastest.
Arguments:
- tokens: bfloat16 [256, 2048], P(('grp', 'dp'), 'ra'), parts along dimension 0, may hold values from -62 to 62
- gain_first: float32 [2048], P('ra'), may hold values from 0.1 to 1.9
- up_first: bfloat16 [2048, 8192], P('ra', 'cb'), may hold values from -0.125 to 0.125
- down_first: bfloat16 [8192, 2048], P('cb', 'ra'), may hold values from -0.0625 to 0.0625
- gain_second: float32 [2048], P('ra'), may hold values from 0.1 to 1.9
- up_second: bfloat16 [2048, 8192], P('ra', 'cb'), may hold values from -0.125 to 0.125
- down_second: bfloat16 [8192, 2048], P('cb', 'ra'), may hold values from -0.0625 to 0.0625
- gain_last: float32 [2048], P('ra'), may hold values from 0.1 to 1.9
Outputs:
- normed: bfloat16 [256, 2048], P(('grp', 'dp'), 'ra'), parts along dimension 0
The draws below stay inside these ranges and needn't reach their ends.
There are 2 independent parts, one for each index of `grp`. The reference program is written for one: setup_inputs(seed, part) draws one part's arguments, and reference() takes and returns one part's arrays. A program takes and returns all parts, laid end to end along the dimension named above; an argument that names none is the same for every part. Nothing has to cross between parts.
All inputs are finite; a program needn't handle non-finite values.
Results may differ from the reference program's by a relative error of at most 0.0095.
Values may be sent and summed in bfloat16 or wider, within the bound.
A program may use at most 64 MiB of HBM per device.

```python
import jax
import jax.numpy as jnp
from jax import lax

D = 2048
FF = 8192
TOKENS = 128


def draw_tokens(key, part):
    key_base = jax.random.fold_in(key, 11)
    key_cols = jax.random.fold_in(key, 12)
    key_rows = jax.random.fold_in(key, 13)
    position = jnp.arange(D, dtype=jnp.float32) / D
    columns = 10.0 ** (position - 0.5) * jnp.exp(jax.random.uniform(key_cols, (D,), jnp.float32, -0.7, 0.7))
    base = jnp.clip(jax.random.normal(key_base, (TOKENS, D), jnp.float32), -6.0, 6.0)
    rows = jnp.exp(jax.random.uniform(key_rows, (TOKENS, 1), jnp.float32, -1.15, 1.15))
    return jnp.clip(base * rows * columns, -62.0, 62.0).astype(jnp.bfloat16)


def steps_of(key, shape, shards, low, high):
    def one(axis_at, blocks):
        steps = jax.random.uniform(jax.random.fold_in(jax.random.fold_in(key, 6), axis_at), (blocks,), jnp.float32, low / len(shards), high / len(shards))
        return jnp.repeat(jnp.exp(steps), shape[axis_at] // blocks).reshape((-1,) + (1,) * (len(shape) - axis_at - 1))

    loudness = one(*shards[0])
    for cut in shards[1:]:
        loudness = loudness * one(*cut)
    return loudness


def normal_values(stream_key, dims, scale, bound, split=(), kind=jnp.bfloat16):
    result = scale * jax.random.normal(stream_key, dims, jnp.float32)
    if split:
        result = result * steps_of(stream_key, dims, split, -0.22, 0.18)
    return jnp.clip(result, -bound, bound).astype(kind)


def setup_inputs(seed: int = 0, part: int = 0) -> dict:
    arg_keys = jax.random.split(jax.random.key(seed), 9)
    part_keys = jax.random.split(jax.random.fold_in(arg_keys[8], part), 9)
    tokens = draw_tokens(jax.random.fold_in(jax.random.fold_in(arg_keys[8], part), 71), part)
    gain_first = jnp.clip(1.0 + 0.18 * jax.random.normal(arg_keys[1], (D,), jnp.float32), 0.1, 1.9)
    up_first = normal_values(arg_keys[2], (D, FF), D ** -0.5, 0.125, ((0, 4), (1, 2)))
    down_first = normal_values(arg_keys[3], (FF, D), FF ** -0.5, 0.0625, ((0, 2), (1, 4)))
    gain_second = jnp.clip(1.0 + 0.18 * jax.random.normal(arg_keys[4], (D,), jnp.float32), 0.1, 1.9)
    up_second = normal_values(arg_keys[5], (D, FF), D ** -0.5, 0.125, ((0, 4), (1, 2)))
    down_second = normal_values(arg_keys[6], (FF, D), FF ** -0.5, 0.0625, ((0, 2), (1, 4)))
    gain_last = jnp.clip(1.0 + 0.18 * jax.random.normal(arg_keys[7], (D,), jnp.float32), 0.1, 1.9)
    return dict(tokens=tokens, gain_first=gain_first, up_first=up_first, down_first=down_first, gain_second=gain_second, up_second=up_second, down_second=down_second, gain_last=gain_last)


EPS = 1e-06

def norm_inverse(h32):
    return lax.rsqrt(lax.optimization_barrier(jnp.mean(h32 * h32, axis=1, keepdims=True)) + EPS)

def mlp_branch(h32, gain, w_up, w_down):
    scaled = (h32 * gain).astype(jnp.bfloat16)
    pre = jnp.dot(scaled, w_up, preferred_element_type=jnp.float32) * norm_inverse(h32)
    hidden = jnp.square(jax.nn.relu(pre)).astype(jnp.bfloat16)
    return jnp.dot(hidden, w_down, preferred_element_type=jnp.float32)

def reference(tokens, gain_first, up_first, down_first, gain_second, up_second, down_second, gain_last):
    start32 = tokens.astype(jnp.float32)
    first = (0.5 * start32 + mlp_branch(start32, gain_first, up_first, down_first)).astype(jnp.bfloat16)
    first32 = first.astype(jnp.float32)
    second = (0.5 * first32 + mlp_branch(first32, gain_second, up_second, down_second)).astype(jnp.bfloat16)
    second32 = second.astype(jnp.float32)
    return (second32 * norm_inverse(second32) * gain_last).astype(jnp.bfloat16)
```

```python
import functools

import jax
import jax.numpy as jnp
from jax import lax
from jax.experimental import pallas as pl
from jax.experimental.pallas import tpu as pltpu
from jax.sharding import PartitionSpec as P

EPS = 1e-06
MESH = pl.DeviceIdType.MESH
F32, BF16 = jnp.float32, jnp.bfloat16

CHUNK = 512
SPLITS = 2
LAG = 4
SLACK = 4


def kernel(
    n,
    ncb,
    width,
    tokens_ref,
    gain_first,
    up_first,
    down_first,
    gain_second,
    up_second,
    down_second,
    gain_last,
    out_ref,
    up_v,
    down_v,
    h_v,
    scaled_v,
    own_v,
    acc_v,
    branch_v,
    inv_v,
    send_v,
    recv_v,
    sq_send,
    sq_recv,
    cb_send,
    cb_recv,
    up_sem,
    down_sem,
    send_sem,
    recv_sem,
    sq_ssem,
    sq_rsem,
    cb_ssem,
    cb_rsem,
):
    k = lax.axis_index("ra")
    cb = lax.axis_index("cb")
    layers, chunks = up_v.shape[0], up_v.shape[1]
    splits, rows = h_v.shape[0], h_v.shape[1]
    chunk = up_v.shape[3]
    jobs = splits * chunks
    early = jnp.where(2 * k < n, 0, 1)
    late = 1 - early
    early_hops = jnp.where(early == 0, k, n - 1 - k)
    has_early = early_hops > 0
    early_to = jnp.where(early == 0, k + 1, k - 1)
    late_to = jnp.where(early_hops > 0, jnp.where(late == 0, k + 1, k - 1), early_to)
    depth = (n - 1 - 2 * early_hops) * LAG
    gap = max(0, chunks + (n - 1) * LAG + SLACK - jobs)

    def up_copy(layer, c):
        ref = (up_first, up_second)[layer]
        return pltpu.make_async_copy(
            ref.at[:, pl.ds(c * chunk, chunk)], up_v.at[layer, c], up_sem.at[layer, c]
        )

    def down_copy(layer, c):
        ref = (down_first, down_second)[layer]
        return pltpu.make_async_copy(
            ref.at[pl.ds(c * chunk, chunk), :], down_v.at[layer, c], down_sem.at[layer, c]
        )

    for layer in range(layers):
        for c in range(chunks):
            up_copy(layer, c).start()
        for c in range(chunks):
            down_copy(layer, c).start()

    barrier = pltpu.get_barrier_semaphore()
    for off in range(1, n):
        pl.semaphore_signal(
            barrier, inc=1, device_id={"ra": lax.rem(k + off, n)}, device_id_type=MESH
        )
    for off in range(1, ncb):
        pl.semaphore_signal(
            barrier, inc=1, device_id={"cb": lax.rem(cb + off, ncb)}, device_id_type=MESH
        )
    pl.semaphore_wait(barrier, n - 1 + ncb - 1)

    def chain(direction, job, to):
        return pltpu.make_async_remote_copy(
            src_ref=send_v.at[direction, job],
            dst_ref=recv_v.at[direction, job],
            send_sem=send_sem.at[direction, job],
            recv_sem=recv_sem.at[direction, job],
            device_id={"ra": to},
            device_id_type=MESH,
        )

    def sq_copy(level, t, source, off, to):
        return pltpu.make_async_remote_copy(
            src_ref=sq_send.at[level, t],
            dst_ref=sq_recv.at[level, t, source],
            send_sem=sq_ssem.at[level, t, off],
            recv_sem=sq_rsem.at[level, t, source],
            device_id={"ra": to},
            device_id_type=MESH,
        )

    def cb_copy(layer, t, source, off, to):
        return pltpu.make_async_remote_copy(
            src_ref=cb_send.at[layer, t],
            dst_ref=cb_recv.at[layer, t, source],
            send_sem=cb_ssem.at[layer, t, off],
            recv_sem=cb_rsem.at[layer, t, source],
            device_id={"cb": to},
            device_id_type=MESH,
        )

    diagonal = lax.broadcasted_iota(jnp.int32, (rows, 128), 0) == lax.broadcasted_iota(
        jnp.int32, (rows, 128), 1
    )

    def send_squares(level, t, h32):
        total = jnp.sum(h32 * h32, axis=1, keepdims=True)
        line = jnp.sum(jnp.where(diagonal, total, 0.0), axis=0, keepdims=True)
        tile = jnp.broadcast_to(line, (8, 128))
        sq_send[level, t] = tile
        sq_recv[level, t, k] = tile
        for off in range(1, n):
            sq_copy(level, t, k, off, lax.rem(k + off, n)).start()

    def inverse_of(level, t):
        for off in range(1, n):
            source = lax.rem(k + off, n)
            sq_copy(level, t, source, off, source).wait_recv()
        total = sq_recv[level, t, 0]
        for source in range(1, n):
            total = total + sq_recv[level, t, source]
        line = lax.rsqrt(total * (1.0 / width) + EPS)[0:1]
        column = jnp.sum(jnp.where(diagonal, line, 0.0), axis=1, keepdims=True)
        return jnp.broadcast_to(column, (rows, 128))

    def gather_branch(layer, t):
        for off in range(1, ncb):
            source = lax.rem(cb + off, ncb)
            cb_copy(layer, t, source, off, source).wait_recv()
        total = cb_recv[layer, t, 0].astype(F32)
        for source in range(1, ncb):
            total = total + cb_recv[layer, t, source].astype(F32)
        return (0.5 * h_v[t] + total).astype(BF16).astype(F32)

    for t in range(splits):
        h32 = tokens_ref[t * rows : (t + 1) * rows, :].astype(F32)
        h_v[t] = h32
        send_squares(0, t, h32)
        scaled_v[0, t] = (h32 * gain_first[...]).astype(BF16)

    def step(s, _):
        level = jnp.where(
            s < jobs + gap, 0, jnp.where(s < 2 * (jobs + gap), 1, 2)
        )
        at = s - level * (jobs + gap)
        live = at < jobs
        t = jnp.where(live, at // chunks, 0)
        c = at % chunks
        job = level * jobs + at

        @pl.when(live & (c == 0) & (level == 1))
        def _():
            h32 = gather_branch(0, t)
            h_v[t] = h32
            send_squares(1, t, h32)
            scaled_v[1, t] = (h32 * gain_second[...]).astype(BF16)

        @pl.when(live & (c == 0) & (level == 2))
        def _():
            h32 = gather_branch(1, t)
            h_v[t] = h32
            send_squares(2, t, h32)

        for layer in range(layers):

            @pl.when(live & (level == layer) & (t == 0))
            def _():
                up_copy(layer, c).wait()

        @pl.when(live & (level < layers))
        def _():
            own = jnp.dot(scaled_v[level, t], up_v[level, c], preferred_element_type=F32)
            own_v[job] = own

            @pl.when(has_early)
            def _():
                chain(early, job, early_to).wait_recv()
                total = recv_v[early, job].astype(F32) + own
                send_v[early, job] = total.astype(BF16)
                acc_v[job] = total

            @pl.when(jnp.logical_not(has_early))
            def _():
                send_v[early, job] = own.astype(BF16)
                acc_v[job] = own

            chain(early, job, early_to).start()

        s2 = s - depth
        level2 = jnp.where(s2 < jobs + gap, 0, 1)
        at2 = s2 - level2 * (jobs + gap)
        live2 = (s2 >= 0) & (at2 < jobs)
        at2 = jnp.where(live2, at2, 0)
        t2 = at2 // chunks
        c2 = at2 % chunks
        job2 = level2 * jobs + at2

        @pl.when(live2 & (c2 == 0))
        def _():
            inv_v[...] = inverse_of(level2, t2)

        for layer in range(layers):

            @pl.when(live2 & (level2 == layer) & (t2 == 0))
            def _():
                down_copy(layer, c2).wait()

        @pl.when(live2)
        def _():
            chain(late, job2, late_to).wait_recv()
            arrived = recv_v[late, job2].astype(F32)

            @pl.when(has_early)
            def _():
                send_v[late, job2] = (arrived + own_v[job2]).astype(BF16)
                chain(late, job2, late_to).start()

            pre = (arrived + acc_v[job2]) * inv_v[:, 0:1]
            hidden = jnp.square(jnp.maximum(pre, 0.0)).astype(BF16)
            part = jnp.dot(hidden, down_v[level2, c2], preferred_element_type=F32)

            @pl.when(c2 == 0)
            def _():
                branch_v[...] = part

            @pl.when(c2 > 0)
            def _():
                branch_v[...] += part

        @pl.when(live2 & (c2 == chunks - 1))
        def _():
            value = branch_v[...].astype(BF16)
            cb_send[level2, t2] = value
            cb_recv[level2, t2, cb] = value
            for off in range(1, ncb):
                cb_copy(level2, t2, cb, off, lax.rem(cb + off, ncb)).start()

        return 0

    lax.fori_loop(0, 2 * (jobs + gap) + (splits - 1) * chunks + 1, step, 0)

    for t in range(splits):
        inv = inverse_of(2, t)[:, 0:1]
        out_ref[t * rows : (t + 1) * rows, :] = (h_v[t] * inv * gain_last[...]).astype(BF16)

    def drain(job, _):
        chain(early, job, early_to).wait_send()

        @pl.when(has_early)
        def _():
            chain(late, job, late_to).wait_send()

        return 0

    lax.fori_loop(0, layers * jobs, drain, 0)
    for t in range(splits):
        for level in range(layers + 1):
            for off in range(1, n):
                sq_copy(level, t, k, off, lax.rem(k + off, n)).wait_send()
        for layer in range(layers):
            for off in range(1, ncb):
                cb_copy(layer, t, cb, off, lax.rem(cb + off, ncb)).wait_send()


def local(n, ncb, *args):
    tokens, gain_first, up_first, down_first, gain_second, up_second, down_second, gain_last = args
    rows, cols = tokens.shape
    hidden = up_first.shape[1]
    chunk = min(CHUNK, hidden)
    chunks = hidden // chunk
    splits = SPLITS if rows % (16 * SPLITS) == 0 else 1
    part = rows // splits
    jobs = 2 * splits * chunks
    vmem = pl.BlockSpec(memory_space=pltpu.VMEM)
    hbm = pl.BlockSpec(memory_space=pl.ANY)
    dma = pltpu.SemaphoreType.DMA
    return pl.pallas_call(
        functools.partial(kernel, n, ncb, cols * n),
        out_shape=jax.ShapeDtypeStruct((rows, cols), BF16),
        in_specs=[vmem, vmem, hbm, hbm, vmem, hbm, hbm, vmem],
        out_specs=vmem,
        scratch_shapes=[
            pltpu.VMEM((2, chunks, cols, chunk), BF16),
            pltpu.VMEM((2, chunks, chunk, cols), BF16),
            pltpu.VMEM((splits, part, cols), F32),
            pltpu.VMEM((2, splits, part, cols), BF16),
            pltpu.VMEM((jobs, part, chunk), F32),
            pltpu.VMEM((jobs, part, chunk), F32),
            pltpu.VMEM((part, cols), F32),
            pltpu.VMEM((part, 128), F32),
            pltpu.VMEM((2, jobs, part, chunk), BF16),
            pltpu.VMEM((2, jobs, part, chunk), BF16),
            pltpu.VMEM((3, splits, 8, 128), F32),
            pltpu.VMEM((3, splits, n, 8, 128), F32),
            pltpu.VMEM((2, splits, part, cols), BF16),
            pltpu.VMEM((2, splits, ncb, part, cols), BF16),
            dma((2, chunks)),
            dma((2, chunks)),
            dma((2, jobs)),
            dma((2, jobs)),
            dma((3, splits, n)),
            dma((3, splits, n)),
            dma((2, splits, ncb)),
            dma((2, splits, ncb)),
        ],
        compiler_params=pltpu.CompilerParams(
            collective_id=0, has_side_effects=True, vmem_limit_bytes=60 * 1024 * 1024
        ),
    )(
        tokens,
        gain_first.reshape(1, cols),
        up_first,
        down_first,
        gain_second.reshape(1, cols),
        up_second,
        down_second,
        gain_last.reshape(1, cols),
    )


def solution(mesh):
    return jax.shard_map(
        functools.partial(local, mesh.shape["ra"], mesh.shape["cb"]),
        mesh=mesh,
        in_specs=(
            P(("grp", "dp"), "ra"),
            P("ra"),
            P("ra", "cb"),
            P("cb", "ra"),
            P("ra"),
            P("ra", "cb"),
            P("cb", "ra"),
            P("ra"),
        ),
        out_specs=P(("grp", "dp"), "ra"),
        check_vma=False,
    )
```

```python
import functools

import jax
import jax.numpy as jnp
from jax import lax
from jax.experimental import pallas as pl
from jax.experimental.pallas import tpu as pltpu
from jax.sharding import PartitionSpec as P

EPS = 1e-06
MESH = pl.DeviceIdType.MESH
F32, BF16 = jnp.float32, jnp.bfloat16

CHUNK = 1024
SPLITS = 4
LAG = 5
SLACK = 4


def kernel(
    n,
    ncb,
    width,
    tokens_ref,
    gain_first,
    up_first,
    down_first,
    gain_second,
    up_second,
    down_second,
    gain_last,
    out_ref,
    tokens_v,
    gain_v,
    out_v,
    up_v,
    down_v,
    h_v,
    scaled_v,
    own_v,
    acc_v,
    branch_v,
    inv_v,
    send_v,
    recv_v,
    sq_send,
    sq_recv,
    cb_send,
    cb_recv,
    in_sem,
    out_sem,
    weight_sem,
    send_sem,
    recv_sem,
    sq_ssem,
    sq_rsem,
    cb_ssem,
    cb_rsem,
):
    k = lax.axis_index("ra")
    cb = lax.axis_index("cb")
    layers, hidden = up_v.shape[0], up_v.shape[2]
    splits, rows = h_v.shape[0], h_v.shape[1]
    chunk = send_v.shape[3]
    chunks = hidden // chunk
    jobs = splits * chunks
    early = jnp.where(2 * k < n, 0, 1)
    late = 1 - early
    early_hops = jnp.where(early == 0, k, n - 1 - k)
    has_early = early_hops > 0
    early_to = jnp.where(early == 0, k + 1, k - 1)
    late_to = jnp.where(early_hops > 0, jnp.where(late == 0, k + 1, k - 1), early_to)
    depth = (n - 1 - 2 * early_hops) * LAG
    gap = max(0, chunks + (n - 1) * LAG + SLACK - jobs)

    def up_copy(layer):
        ref = (up_first, up_second)[layer]
        return pltpu.make_async_copy(ref, up_v.at[layer], weight_sem.at[layer])

    def down_copy(layer):
        ref = (down_first, down_second)[layer]
        return pltpu.make_async_copy(ref, down_v.at[layer], weight_sem.at[layers + layer])

    inputs = [pltpu.make_async_copy(tokens_ref, tokens_v, in_sem.at[0])]
    for i, ref in enumerate((gain_first, gain_second, gain_last)):
        inputs.append(pltpu.make_async_copy(ref, gain_v.at[i], in_sem.at[1 + i]))
    for copy in inputs:
        copy.start()
    up_copy(0).start()

    barrier = pltpu.get_barrier_semaphore()
    for off in range(1, n):
        pl.semaphore_signal(
            barrier, inc=1, device_id={"ra": lax.rem(k + off, n)}, device_id_type=MESH
        )
    for off in range(1, ncb):
        pl.semaphore_signal(
            barrier, inc=1, device_id={"cb": lax.rem(cb + off, ncb)}, device_id_type=MESH
        )
    for copy in inputs:
        copy.wait()
    for t in range(splits):
        h32 = tokens_v[t * rows : (t + 1) * rows, :].astype(F32)
        h_v[t] = h32
        scaled_v[0, t] = (h32 * gain_v[0]).astype(BF16)
    pl.semaphore_wait(barrier, n - 1 + ncb - 1)
    down_copy(0).start()
    up_copy(1).start()
    down_copy(1).start()

    def chain(direction, job, to):
        return pltpu.make_async_remote_copy(
            src_ref=send_v.at[direction, job],
            dst_ref=recv_v.at[direction, job],
            send_sem=send_sem.at[direction],
            recv_sem=recv_sem.at[direction, lax.rem(job, jobs)],
            device_id={"ra": to},
            device_id_type=MESH,
        )

    def sq_copy(level, t, source, to):
        return pltpu.make_async_remote_copy(
            src_ref=sq_send.at[level, t],
            dst_ref=sq_recv.at[level, t, source],
            send_sem=sq_ssem,
            recv_sem=sq_rsem.at[level, t],
            device_id={"ra": to},
            device_id_type=MESH,
        )

    def cb_copy(layer, t, source, to):
        return pltpu.make_async_remote_copy(
            src_ref=cb_send.at[layer, t],
            dst_ref=cb_recv.at[layer, t, source],
            send_sem=cb_ssem,
            recv_sem=cb_rsem.at[layer, t],
            device_id={"cb": to},
            device_id_type=MESH,
        )

    def of_all(ref, ssem, rsem, axis, to):
        return pltpu.make_async_remote_copy(
            src_ref=ref,
            dst_ref=ref,
            send_sem=ssem,
            recv_sem=rsem,
            device_id={axis: to},
            device_id_type=MESH,
        )

    diagonal = lax.broadcasted_iota(jnp.int32, (rows, 128), 0) == lax.broadcasted_iota(
        jnp.int32, (rows, 128), 1
    )

    def send_squares(level, t, h32):
        total = jnp.sum(h32 * h32, axis=1, keepdims=True)
        line = jnp.sum(jnp.where(diagonal, total, 0.0), axis=0, keepdims=True)
        sq_send[level, t] = line
        sq_recv[level, t, k] = line
        for off in range(1, n):
            sq_copy(level, t, k, lax.rem(k + off, n)).start()

    def inverse_of(level, t):
        peers = sq_recv.at[level, t, pl.ds(0, n - 1)]
        of_all(peers, sq_ssem, sq_rsem.at[level, t], "ra", lax.rem(k + 1, n)).wait_recv()
        total = sq_recv[level, t, 0]
        for source in range(1, n):
            total = total + sq_recv[level, t, source]
        line = lax.rsqrt(total * (1.0 / width) + EPS)
        column = jnp.sum(jnp.where(diagonal, line, 0.0), axis=1, keepdims=True)
        return jnp.broadcast_to(column, (rows, 128))

    def gather_branch(layer, t):
        peers = cb_recv.at[layer, t, pl.ds(0, ncb - 1)]
        of_all(peers, cb_ssem, cb_rsem.at[layer, t], "cb", lax.rem(cb + 1, ncb)).wait_recv()
        total = cb_recv[layer, t, 0].astype(F32)
        for source in range(1, ncb):
            total = total + cb_recv[layer, t, source].astype(F32)
        return (0.5 * h_v[t] + total).astype(BF16).astype(F32)

    for t in range(splits):
        send_squares(0, t, h_v[t])

    def step(s, _):
        level = jnp.where(
            s < jobs + gap, 0, jnp.where(s < 2 * (jobs + gap), 1, 2)
        )
        at = s - level * (jobs + gap)
        live = at < jobs
        t = jnp.where(live, at // chunks, 0)
        c = at % chunks
        job = level * jobs + at

        @pl.when(live & (c == 0) & (level == 1))
        def _():
            h32 = gather_branch(0, t)
            h_v[t] = h32
            send_squares(1, t, h32)
            scaled_v[1, t] = (h32 * gain_v[1]).astype(BF16)

        @pl.when(live & (c == 0) & (level == 2))
        def _():
            h32 = gather_branch(1, t)
            h_v[t] = h32
            send_squares(2, t, h32)

        for layer in range(layers):

            @pl.when((level == layer) & (at == 0))
            def _():
                up_copy(layer).wait()

        @pl.when(live & (level < layers))
        def _():
            own = jnp.dot(scaled_v[level, t], up_v[level, :, pl.ds(pl.multiple_of(c * chunk, chunk), chunk)], preferred_element_type=F32)
            own_v[job] = own

            @pl.when(has_early)
            def _():
                chain(early, job, early_to).wait_recv()
                total = recv_v[early, job].astype(F32) + own
                send_v[early, job] = total.astype(BF16)
                acc_v[job] = total

            @pl.when(jnp.logical_not(has_early))
            def _():
                send_v[early, job] = own.astype(BF16)
                acc_v[job] = own

            chain(early, job, early_to).start()

        s2 = s - depth
        level2 = jnp.where(s2 < jobs + gap, 0, 1)
        at2 = s2 - level2 * (jobs + gap)
        live2 = (s2 >= 0) & (at2 < jobs)
        at2 = jnp.where(live2, at2, 0)
        t2 = at2 // chunks
        c2 = at2 % chunks
        job2 = level2 * jobs + at2

        @pl.when(live2 & (c2 == 0))
        def _():
            inv_v[...] = inverse_of(level2, t2)

        for layer in range(layers):

            @pl.when(live2 & (job2 == layer * jobs))
            def _():
                down_copy(layer).wait()

        @pl.when(live2)
        def _():
            chain(late, job2, late_to).wait_recv()
            arrived = recv_v[late, job2].astype(F32)

            @pl.when(has_early)
            def _():
                send_v[late, job2] = (arrived + own_v[job2]).astype(BF16)
                chain(late, job2, late_to).start()

            pre = (arrived + acc_v[job2]) * inv_v[:, 0:1]
            hidden = jnp.square(jnp.maximum(pre, 0.0)).astype(BF16)
            part = jnp.dot(hidden, down_v[level2, pl.ds(pl.multiple_of(c2 * chunk, chunk), chunk), :], preferred_element_type=F32)

            @pl.when(c2 == 0)
            def _():
                branch_v[...] = part

            @pl.when(c2 > 0)
            def _():
                branch_v[...] += part

        @pl.when(live2 & (c2 == chunks - 1))
        def _():
            value = branch_v[...].astype(BF16)
            cb_send[level2, t2] = value
            cb_recv[level2, t2, cb] = value
            for off in range(1, ncb):
                cb_copy(level2, t2, cb, lax.rem(cb + off, ncb)).start()

        return 0

    lax.fori_loop(0, 2 * (jobs + gap) + (splits - 1) * chunks + 1, step, 0)

    def out_copy():
        return pltpu.make_async_copy(out_v, out_ref, out_sem)

    for t in range(splits):
        inv = inverse_of(2, t)[:, 0:1]
        out_v[t * rows : (t + 1) * rows, :] = (h_v[t] * inv * gain_v[2]).astype(BF16)
    out_copy().start()

    of_all(send_v.at[early], send_sem.at[early], recv_sem.at[early, 0], "ra", early_to).wait_send()

    @pl.when(has_early)
    def _():
        of_all(send_v.at[late], send_sem.at[late], recv_sem.at[late, 0], "ra", late_to).wait_send()

    peers = sq_recv.at[:, :, pl.ds(0, n - 1)]
    of_all(peers, sq_ssem, sq_rsem.at[0, 0], "ra", lax.rem(k + 1, n)).wait_send()
    peers = cb_recv.at[:, :, pl.ds(0, ncb - 1)]
    of_all(peers, cb_ssem, cb_rsem.at[0, 0], "cb", lax.rem(cb + 1, ncb)).wait_send()
    out_copy().wait()


def local(n, ncb, *args):
    tokens, gain_first, up_first, down_first, gain_second, up_second, down_second, gain_last = args
    rows, cols = tokens.shape
    hidden = up_first.shape[1]
    chunk = min(CHUNK, hidden)
    chunks = hidden // chunk
    splits = SPLITS if rows % (16 * SPLITS) == 0 else 1
    part = rows // splits
    jobs = 2 * splits * chunks
    hbm = pl.BlockSpec(memory_space=pl.ANY)
    dma = pltpu.SemaphoreType.DMA
    return pl.pallas_call(
        functools.partial(kernel, n, ncb, cols * n),
        out_shape=jax.ShapeDtypeStruct((rows, cols), BF16),
        in_specs=[hbm] * 8,
        out_specs=hbm,
        scratch_shapes=[
            pltpu.VMEM((rows, cols), BF16),
            pltpu.VMEM((3, 1, cols), F32),
            pltpu.VMEM((rows, cols), BF16),
            pltpu.VMEM((2, cols, hidden), BF16),
            pltpu.VMEM((2, hidden, cols), BF16),
            pltpu.VMEM((splits, part, cols), F32),
            pltpu.VMEM((2, splits, part, cols), BF16),
            pltpu.VMEM((jobs, part, chunk), F32),
            pltpu.VMEM((jobs, part, chunk), F32),
            pltpu.VMEM((part, cols), F32),
            pltpu.VMEM((part, 128), F32),
            pltpu.VMEM((2, jobs, part, chunk), BF16),
            pltpu.VMEM((2, jobs, part, chunk), BF16),
            pltpu.VMEM((3, splits, 1, 128), F32),
            pltpu.VMEM((3, splits, n, 1, 128), F32),
            pltpu.VMEM((2, splits, part, cols), BF16),
            pltpu.VMEM((2, splits, ncb, part, cols), BF16),
            dma((4,)),
            dma,
            dma((4,)),
            dma((2,)),
            dma((2, jobs // 2)),
            dma,
            dma((3, splits)),
            dma,
            dma((2, splits)),
        ],
        compiler_params=pltpu.CompilerParams(
            collective_id=0, has_side_effects=True, vmem_limit_bytes=60 * 1024 * 1024
        ),
    )(
        tokens,
        gain_first.reshape(1, cols),
        up_first,
        down_first,
        gain_second.reshape(1, cols),
        up_second,
        down_second,
        gain_last.reshape(1, cols),
    )


def solution(mesh):
    return jax.shard_map(
        functools.partial(local, mesh.shape["ra"], mesh.shape["cb"]),
        mesh=mesh,
        in_specs=(
            P(("grp", "dp"), "ra"),
            P("ra"),
            P("ra", "cb"),
            P("cb", "ra"),
            P("ra"),
            P("ra", "cb"),
            P("cb", "ra"),
            P("ra"),
        ),
        out_specs=P(("grp", "dp"), "ra"),
        check_vma=False,
    )
```

```python
import functools

import jax
import jax.numpy as jnp
from jax import lax
from jax.experimental import pallas as pl
from jax.experimental.pallas import tpu as pltpu
from jax.sharding import PartitionSpec as P

EPS = 1e-06
MESH = pl.DeviceIdType.MESH
F32, BF16 = jnp.float32, jnp.bfloat16

CHUNK = 1024
SPLITS = 4
LAG = 5
SLACK = 3


def kernel(
    n,
    ncb,
    width,
    tokens_ref,
    gain_first,
    up_first,
    down_first,
    gain_second,
    up_second,
    down_second,
    gain_last,
    out_ref,
    tokens_v,
    gain_v,
    out_v,
    up_v,
    down_v,
    h_v,
    scaled_v,
    own_v,
    acc_v,
    branch_v,
    inv_v,
    send_v,
    recv_v,
    sq_send,
    sq_recv,
    cb_send,
    cb_recv,
    in_sem,
    out_sem,
    weight_sem,
    send_sem,
    recv_sem,
    sq_ssem,
    sq_rsem,
    cb_ssem,
    cb_rsem,
):
    k = lax.axis_index("ra")
    cb = lax.axis_index("cb")
    layers, hidden = up_v.shape[0], up_v.shape[2]
    splits, rows = h_v.shape[0], h_v.shape[1]
    chunk = send_v.shape[3]
    chunks = hidden // chunk
    jobs = splits * chunks
    early = jnp.where(2 * k < n, 0, 1)
    late = 1 - early
    early_hops = jnp.where(early == 0, k, n - 1 - k)
    has_early = early_hops > 0
    early_to = jnp.where(early == 0, k + 1, k - 1)
    late_to = jnp.where(early_hops > 0, jnp.where(late == 0, k + 1, k - 1), early_to)
    depth = jnp.maximum((n - 1 - 2 * early_hops) * LAG, 1)
    gap = max(0, chunks + (n - 1) * LAG + SLACK - jobs)

    def up_copy(layer):
        ref = (up_first, up_second)[layer]
        return pltpu.make_async_copy(ref, up_v.at[layer], weight_sem.at[layer])

    def down_copy(layer):
        ref = (down_first, down_second)[layer]
        return pltpu.make_async_copy(ref, down_v.at[layer], weight_sem.at[layers + layer])

    inputs = [pltpu.make_async_copy(tokens_ref, tokens_v, in_sem.at[0])]
    for i, ref in enumerate((gain_first, gain_second, gain_last)):
        inputs.append(pltpu.make_async_copy(ref, gain_v.at[i], in_sem.at[1 + i]))
    for copy in inputs:
        copy.start()
    up_copy(0).start()

    barrier = pltpu.get_barrier_semaphore()
    for off in range(1, n):
        pl.semaphore_signal(
            barrier, inc=1, device_id={"ra": lax.rem(k + off, n)}, device_id_type=MESH
        )
    for off in range(1, ncb):
        pl.semaphore_signal(
            barrier, inc=1, device_id={"cb": lax.rem(cb + off, ncb)}, device_id_type=MESH
        )
    for copy in inputs:
        copy.wait()
    for t in range(splits):
        h32 = tokens_v[t * rows : (t + 1) * rows, :].astype(F32)
        h_v[t] = h32
        scaled_v[0, t] = (h32 * gain_v[0]).astype(BF16)
    pl.semaphore_wait(barrier, n - 1 + ncb - 1)
    down_copy(0).start()
    up_copy(1).start()
    down_copy(1).start()

    def chain(direction, job, to):
        return pltpu.make_async_remote_copy(
            src_ref=send_v.at[direction, job],
            dst_ref=recv_v.at[direction, job],
            send_sem=send_sem.at[direction],
            recv_sem=recv_sem.at[direction, lax.rem(job, jobs)],
            device_id={"ra": to},
            device_id_type=MESH,
        )

    def sq_copy(level, t, source, to):
        return pltpu.make_async_remote_copy(
            src_ref=sq_send.at[level, t],
            dst_ref=sq_recv.at[level, t, source],
            send_sem=sq_ssem,
            recv_sem=sq_rsem.at[level, t],
            device_id={"ra": to},
            device_id_type=MESH,
        )

    def cb_copy(layer, t, source, to):
        return pltpu.make_async_remote_copy(
            src_ref=cb_send.at[layer, t],
            dst_ref=cb_recv.at[layer, t, source],
            send_sem=cb_ssem,
            recv_sem=cb_rsem.at[layer, t],
            device_id={"cb": to},
            device_id_type=MESH,
        )

    def of_all(ref, ssem, rsem, axis, to):
        return pltpu.make_async_remote_copy(
            src_ref=ref,
            dst_ref=ref,
            send_sem=ssem,
            recv_sem=rsem,
            device_id={axis: to},
            device_id_type=MESH,
        )

    diagonal = lax.broadcasted_iota(jnp.int32, (rows, 128), 0) == lax.broadcasted_iota(
        jnp.int32, (rows, 128), 1
    )

    def send_squares(level, t, h32):
        total = jnp.sum(h32 * h32, axis=1, keepdims=True)
        line = jnp.sum(jnp.where(diagonal, total, 0.0), axis=0, keepdims=True)
        sq_send[level, t] = line
        sq_recv[level, t, k] = line
        for off in range(1, n):
            sq_copy(level, t, k, lax.rem(k + off, n)).start()

    def inverse_of(level, t):
        peers = sq_recv.at[level, t, pl.ds(0, n - 1)]
        of_all(peers, sq_ssem, sq_rsem.at[level, t], "ra", lax.rem(k + 1, n)).wait_recv()
        total = sq_recv[level, t, 0]
        for source in range(1, n):
            total = total + sq_recv[level, t, source]
        line = lax.rsqrt(total * (1.0 / width) + EPS)
        column = jnp.sum(jnp.where(diagonal, line, 0.0), axis=1, keepdims=True)
        return jnp.broadcast_to(column, (rows, 128))

    def gather_branch(layer, t):
        peers = cb_recv.at[layer, t, pl.ds(0, ncb - 1)]
        of_all(peers, cb_ssem, cb_rsem.at[layer, t], "cb", lax.rem(cb + 1, ncb)).wait_recv()
        total = cb_recv[layer, t, 0].astype(F32)
        for source in range(1, ncb):
            total = total + cb_recv[layer, t, source].astype(F32)
        return (0.5 * h_v[t] + total).astype(BF16).astype(F32)

    for t in range(splits):
        send_squares(0, t, h_v[t])

    def multiply_up(level, t, c):
        columns = pl.ds(pl.multiple_of(c * chunk, chunk), chunk)
        own_v[(level * splits + t) * chunks + c] = jnp.dot(
            scaled_v[level, t], up_v[level, :, columns], preferred_element_type=F32
        )

    up_copy(0).wait()
    multiply_up(0, 0, 0)

    def step(s, _):
        s2 = s - depth
        level2 = jnp.where(s2 < jobs + gap, 0, 1)
        at2 = s2 - level2 * (jobs + gap)
        live2 = (s2 >= 0) & (at2 < jobs)
        at2 = jnp.where(live2, at2, 0)
        t2 = at2 // chunks
        c2 = at2 % chunks
        job2 = level2 * jobs + at2

        @pl.when(live2)
        def _():
            chain(late, job2, late_to).wait_recv()

            @pl.when(has_early)
            def _():
                send_v[late, job2] = (recv_v[late, job2].astype(F32) + own_v[job2]).astype(BF16)
                chain(late, job2, late_to).start()

        @pl.when(live2 & (c2 == 0))
        def _():
            inv_v[...] = inverse_of(level2, t2)

        for layer in range(layers):

            @pl.when(live2 & (job2 == layer * jobs))
            def _():
                down_copy(layer).wait()

        @pl.when(live2)
        def _():
            pre = (recv_v[late, job2].astype(F32) + acc_v[job2]) * inv_v[:, 0:1]
            hidden = jnp.square(jnp.maximum(pre, 0.0)).astype(BF16)
            rows_at = pl.ds(pl.multiple_of(c2 * chunk, chunk), chunk)
            part = jnp.dot(hidden, down_v[level2, rows_at, :], preferred_element_type=F32)

            @pl.when(c2 == 0)
            def _():
                branch_v[...] = part

            @pl.when(c2 > 0)
            def _():
                branch_v[...] += part

        @pl.when(live2 & (c2 == chunks - 1))
        def _():
            value = branch_v[...].astype(BF16)
            cb_send[level2, t2] = value
            cb_recv[level2, t2, cb] = value
            for off in range(1, ncb):
                cb_copy(level2, t2, cb, lax.rem(cb + off, ncb)).start()

        level = jnp.where(
            s < jobs + gap, 0, jnp.where(s < 2 * (jobs + gap), 1, 2)
        )
        at = s - level * (jobs + gap)
        live = at < jobs
        t = jnp.where(live, at // chunks, 0)
        c = at % chunks
        job = level * jobs + at

        @pl.when(live & (c == 0) & (level == 1))
        def _():
            h32 = gather_branch(0, t)
            h_v[t] = h32
            send_squares(1, t, h32)
            scaled_v[1, t] = (h32 * gain_v[1]).astype(BF16)

            @pl.when(at == 0)
            def _():
                up_copy(1).wait()

            multiply_up(1, t, 0)

        @pl.when(live & (c == 0) & (level == 2))
        def _():
            h32 = gather_branch(1, t)
            h_v[t] = h32
            send_squares(2, t, h32)

        @pl.when(live & (level < layers))
        def _():
            own = own_v[job]

            @pl.when(has_early)
            def _():
                chain(early, job, early_to).wait_recv()
                total = recv_v[early, job].astype(F32) + own
                send_v[early, job] = total.astype(BF16)
                acc_v[job] = total

            @pl.when(jnp.logical_not(has_early))
            def _():
                send_v[early, job] = own.astype(BF16)
                acc_v[job] = own

            chain(early, job, early_to).start()

        follows = (level < layers) & (at + 1 < jobs)
        near = jnp.where(follows, at + 1, 0)

        @pl.when(follows & ((level == 0) | (near % chunks > 0)))
        def _():
            multiply_up(level, near // chunks, near % chunks)

        return 0

    lax.fori_loop(0, 2 * (jobs + gap) + (splits - 1) * chunks + 1, step, 0)

    def out_copy():
        return pltpu.make_async_copy(out_v, out_ref, out_sem)

    for t in range(splits):
        inv = inverse_of(2, t)[:, 0:1]
        out_v[t * rows : (t + 1) * rows, :] = (h_v[t] * inv * gain_v[2]).astype(BF16)
    out_copy().start()

    of_all(send_v.at[early], send_sem.at[early], recv_sem.at[early, 0], "ra", early_to).wait_send()

    @pl.when(has_early)
    def _():
        of_all(send_v.at[late], send_sem.at[late], recv_sem.at[late, 0], "ra", late_to).wait_send()

    peers = sq_recv.at[:, :, pl.ds(0, n - 1)]
    of_all(peers, sq_ssem, sq_rsem.at[0, 0], "ra", lax.rem(k + 1, n)).wait_send()
    peers = cb_recv.at[:, :, pl.ds(0, ncb - 1)]
    of_all(peers, cb_ssem, cb_rsem.at[0, 0], "cb", lax.rem(cb + 1, ncb)).wait_send()
    out_copy().wait()


def local(n, ncb, *args):
    tokens, gain_first, up_first, down_first, gain_second, up_second, down_second, gain_last = args
    rows, cols = tokens.shape
    hidden = up_first.shape[1]
    chunk = min(CHUNK, hidden)
    chunks = hidden // chunk
    splits = SPLITS if rows % (16 * SPLITS) == 0 else 1
    part = rows // splits
    jobs = 2 * splits * chunks
    hbm = pl.BlockSpec(memory_space=pl.ANY)
    dma = pltpu.SemaphoreType.DMA
    return pl.pallas_call(
        functools.partial(kernel, n, ncb, cols * n),
        out_shape=jax.ShapeDtypeStruct((rows, cols), BF16),
        in_specs=[hbm] * 8,
        out_specs=hbm,
        scratch_shapes=[
            pltpu.VMEM((rows, cols), BF16),
            pltpu.VMEM((3, 1, cols), F32),
            pltpu.VMEM((rows, cols), BF16),
            pltpu.VMEM((2, cols, hidden), BF16),
            pltpu.VMEM((2, hidden, cols), BF16),
            pltpu.VMEM((splits, part, cols), F32),
            pltpu.VMEM((2, splits, part, cols), BF16),
            pltpu.VMEM((jobs, part, chunk), F32),
            pltpu.VMEM((jobs, part, chunk), F32),
            pltpu.VMEM((part, cols), F32),
            pltpu.VMEM((part, 128), F32),
            pltpu.VMEM((2, jobs, part, chunk), BF16),
            pltpu.VMEM((2, jobs, part, chunk), BF16),
            pltpu.VMEM((3, splits, 1, 128), F32),
            pltpu.VMEM((3, splits, n, 1, 128), F32),
            pltpu.VMEM((2, splits, part, cols), BF16),
            pltpu.VMEM((2, splits, ncb, part, cols), BF16),
            dma((4,)),
            dma,
            dma((4,)),
            dma((2,)),
            dma((2, jobs // 2)),
            dma,
            dma((3, splits)),
            dma,
            dma((2, splits)),
        ],
        compiler_params=pltpu.CompilerParams(
            collective_id=0, has_side_effects=True, vmem_limit_bytes=60 * 1024 * 1024
        ),
    )(
        tokens,
        gain_first.reshape(1, cols),
        up_first,
        down_first,
        gain_second.reshape(1, cols),
        up_second,
        down_second,
        gain_last.reshape(1, cols),
    )


def solution(mesh):
    return jax.shard_map(
        functools.partial(local, mesh.shape["ra"], mesh.shape["cb"]),
        mesh=mesh,
        in_specs=(
            P(("grp", "dp"), "ra"),
            P("ra"),
            P("ra", "cb"),
            P("cb", "ra"),
            P("ra"),
            P("ra", "cb"),
            P("cb", "ra"),
            P("ra"),
        ),
        out_specs=P(("grp", "dp"), "ra"),
        check_vma=False,
    )
```
